32 devices in a mesh: grp: 2 (over y), sp: 4 (over z), tp: 4 (over x, core).
Axes of the slice: x: 2, y: 2, z: 4, core: 2. Of those that a mesh axis runs over, the one named last changes fastest.
Arguments:
- queries: bfloat16 [1024, 2048], P(('grp', 'sp'), 'tp'), parts along dimension 0, may hold values from -8 to 8
- keys: bfloat16 [1024, 1024], P(('grp', 'sp'), 'tp'), parts along dimension 0, may hold values from -6 to 6
- values: bfloat16 [1024, 1024], P(('grp', 'sp'), 'tp'), parts along dimension 0, may hold values from -6 to 6
- head_bias: float32 [16], P('tp'), may hold values from -15 to -5
- documents: int32 [1024], P(('grp', 'sp')), parts along dimension 0, may hold values from 0 to 2, never falling along the last dimension, each value on 1 to 384 neighbouring positions
- w_out: bfloat16 [2048, 2048], P('tp'), may hold values from -0.125 to 0.125
- resid: bfloat16 [1024, 2048], P(('grp', 'sp', 'tp')), parts along dimension 0, may hold values from -6 to 6
- norm_gain: float32 [2048], replicated, may hold values from 0.1 to 1.9
- expert_ids: int32 [1024, 2], P(('grp', 'sp', 'tp')), parts along dimension 0, may hold values from 0 to 3, all different within a row; in each aligned block of 32 rows (0 to 31, 32 to 63, ...) at most 32 rows name the same one
- expert_gates: float32 [1024, 2], P(('grp', 'sp', 'tp')), parts along dimension 0, may hold values from 0.1 to 0.9
- w_gate: bfloat16 [4, 2048, 3072], P('sp', None, 'tp'), may hold values from -0.125 to 0.125
- w_up: bfloat16 [4, 2048, 3072], P('sp', None, 'tp'), may hold values from -0.125 to 0.125
- w_down: bfloat16 [4, 3072, 2048], P('sp', 'tp'), may hold values from -0.109375 to 0.109375
Outputs:
- layer_out: bfloat16 [1024, 2048], P(('grp', 'sp', 'tp')), parts along dimension 0
The draws below stay inside these ranges and needn't reach their ends.
There are 2 independent parts, one for each index of `grp`. The reference program is written for one: setup_inputs(seed, part) draws one part's arguments, and reference() takes and returns one part's arrays. A program takes and returns all parts, laid end to end along the dimension named above; an argument that names none is the same for every part. Nothing has to cross between parts.
Inputs may be any that keep to these rules, and one draw needn't show every extreme that they name: Document numbers never fall along the sequence; each of the 3 documents holds at least one position and the longest exactly 384 positions. `expert_ids`: each position names 2 different experts. Among the 32 positions of one device (aligned blocks of 32 rows) no expert is named more than 32 times, and in some block some expert exactly 32 times.
All inputs are finite; a program needn't handle non-finite values.
Results may differ from the reference program's by a relative error of at most 0.012.
Values may be sent and summed in bfloat16 or wider, within the bound.
A program may use at most 64 MiB of HBM per device.

```python
import math
import jax
import jax.numpy as jnp
import numpy as np
from jax import lax

D = 2048
HEADS = 16
KV_HEADS = 8
DH = 128
FF = 3072
TOPK = 2
DOCS = 3
SEQ = 512
ROWS = 32
EXPERTS = 4
CAP = 32
N_SP = 4
N_TP = 4


def draw_head_bias(key, part):
    return jax.random.uniform(key, (HEADS,), jnp.float32, -14.0, -5.0)


def shard_levels(own_key, dims, split, least, largest):
    gain, own = 1.0, jax.random.fold_in(own_key, 6)
    for axis_at, parts in split:
        steps = jnp.exp(jax.random.uniform(jax.random.fold_in(own, axis_at), (parts,), jnp.float32, least / len(split), largest / len(split)))
        gain = gain * jnp.repeat(steps, dims[axis_at] // parts).reshape([-1 if axis == axis_at else 1 for axis in range(len(dims))])
    return gain


def split_up(amount, total, reach, lean):
    loads = [(1 << 20) // math.isqrt(rank ** lean) + 1 for rank in range(2, amount + 1)]
    spare, holding = total - reach - (amount - 1), [1] * (amount - 1)
    while spare > 0:
        free = [i for i in range(amount - 1) if holding[i] < reach]
        whole, remaining = sum([loads[i] for i in free]), spare
        for i in free:
            extra = min(reach - holding[i], max(1, remaining * loads[i] // whole), spare)
            holding[i] = holding[i] + extra
            spare = spare - extra
    return np.array([reach] + holding)


def ragged_sizes(rng, count, total, reach, slope):
    if count == 2:
        one = jax.random.randint(rng, (), max(1, total - reach), min(reach, total - 1) + 1)
        return jnp.stack([one, total - one])
    sizes = jnp.asarray(split_up(count, total, reach, slope), jnp.int32)
    couples = (count - 1) // 2
    giver, taker = sizes[1:1 + 2 * couples:2], sizes[2:2 + 2 * couples:2]
    slack = jnp.minimum(giver - 1, reach - taker)
    shifted = jax.random.randint(jax.random.fold_in(rng, 1), (couples,), 0, 1 << 20) % (slack + 1)
    sizes = sizes.at[1:1 + 2 * couples:2].set(giver - shifted).at[2:2 + 2 * couples:2].set(taker + shifted)
    return sizes[jax.random.permutation(jax.random.fold_in(rng, 2), count)]


def assign_block(own_key, own, number, rows, number_of, top, most, slope):
    order = jax.random.permutation(own_key, number_of)
    packed, common = shares(number_of, rows * top, most, slope, True), shares(number_of, rows * top, most, slope, False)
    places = jnp.arange(number_of)

    def named(tallies, offset_by):
        used = int((tallies > 0).sum())
        fixed = max(1, used // 4)
        shifted = fixed + (places - fixed + offset_by * (used - fixed)) % max(1, number_of - fixed)
        return jnp.zeros((number_of,), jnp.int32).at[order[jnp.where(places < fixed, places, shifted)]].set(jnp.asarray(tallies, jnp.int32))

    tallies = jnp.where(number % 4 == 0, named(packed, number // 4), named(common, number - number // 4 - 1))
    mixed = jax.random.permutation(jax.random.fold_in(own, 3), number_of)
    donor, taker = mixed[0:number_of // 2 * 2:2], mixed[1:number_of // 2 * 2:2]
    room = jnp.minimum(tallies[donor] - 1, most - tallies[taker]) // 2
    room = jnp.where((donor == order[0]) | (taker == order[0]) | (tallies[taker] == 0), 0, jnp.maximum(room, 0))
    shifted = jax.random.randint(jax.random.fold_in(own, 4), (number_of // 2,), 0, 1 << 20) % (room + 1)
    tallies = tallies.at[donor].add(-shifted).at[taker].add(shifted)
    labels = jnp.searchsorted(jnp.cumsum(tallies), jnp.arange(rows * top), side="right").astype(jnp.int32)
    table = labels.reshape(top, rows).T
    table = table[jax.random.permutation(jax.random.fold_in(own, 1), rows)]
    offset_by = jax.random.randint(jax.random.fold_in(own, 2), (rows, 1), 0, top)
    return jnp.take_along_axis(table, (jnp.arange(top)[None, :] + offset_by) % top, axis=1)


def shares(amount, total, reach, skew, full):
    loads = [(1 << 20) // math.isqrt(grade ** skew) + 1 for grade in range(1, amount + 1)]
    largest = reach if full else min(reach, max(-(-total // amount), total * loads[0] // sum(loads)))
    least = 1 if total - largest >= amount - 1 else 0
    given, rest = [largest] + [least] * (amount - 1), total - largest - least * (amount - 1)
    while rest > 0:
        candidates = [i for i in range(1, amount) if given[i] < largest] or [i for i in range(1, amount) if given[i] < reach]
        whole, budget = sum([loads[i] for i in candidates]), rest
        for i in candidates:
            extra = min(reach - given[i], max(1, budget * loads[i] // whole), rest)
            given[i] = given[i] + extra
            rest = rest - extra
    return np.array(given)


def centred(own_key, shape, width, most, split=(), kind=jnp.bfloat16):
    result = jax.random.normal(own_key, shape, jnp.float32) * width
    if len(split) > 0:
        result = shard_levels(own_key, shape, split, -0.22, 0.18) * result
    return jnp.clip(result, min=-most, max=most).astype(kind)


def setup_inputs(seed: int = 0, part: int = 0) -> dict:
    key_list = jax.random.split(jax.random.key(seed), 14)
    own_keys = jax.random.split(jax.random.fold_in(key_list[13], part), 14)
    queries = centred(own_keys[0], (SEQ, HEADS * DH), 2.0, 8.0, ((0, 4), (1, 4)))
    keys = centred(own_keys[1], (SEQ, KV_HEADS * DH), 1.0, 6.0, ((0, 4), (1, 4)))
    values = centred(own_keys[2], (SEQ, KV_HEADS * DH), 1.0, 6.0, ((0, 4), (1, 4)))
    head_bias = draw_head_bias(jax.random.fold_in(key_list[13], 71), part)
    documents = jnp.searchsorted(jnp.cumsum(ragged_sizes(own_keys[4], DOCS, SEQ, 3 * SEQ // 4, 0)), jnp.arange(SEQ), side="right").astype(jnp.int32)
    w_out = centred(key_list[5], (HEADS * DH, D), (HEADS * DH) ** -0.5, 0.125, ((0, 4),))
    resid = centred(own_keys[6], (SEQ, D), 1.0, 6.0, ((0, 16),))
    norm_gain = jnp.clip(1.0 + 0.18 * jax.random.normal(key_list[7], (D,), jnp.float32), 0.1, 1.9)
    expert_ids_keys = jax.random.split(jax.random.fold_in(own_keys[8], 1), SEQ // ROWS)
    expert_ids_turns = jax.random.permutation(jax.random.fold_in(own_keys[8], 3), SEQ // ROWS)
    expert_ids = jax.vmap(lambda own, number: assign_block(jax.random.fold_in(own_keys[8], 2), own, number, ROWS, EXPERTS, TOPK, CAP, 1))(expert_ids_keys, expert_ids_turns).reshape((SEQ, TOPK))
    expert_gates = jnp.clip(0.1 + 0.79999997 * jax.random.uniform(own_keys[9], (SEQ, TOPK), jnp.float32) ** shard_levels(own_keys[9], (SEQ, TOPK), ((0, 16),), -0.2, 0.2), 0.1, 0.9)
    w_gate = centred(key_list[10], (EXPERTS, D, FF), D ** -0.5, 0.125, ((0, 4), (2, 4)))
    w_up = centred(key_list[11], (EXPERTS, D, FF), D ** -0.5, 0.125, ((0, 4), (2, 4)))
    w_down = centred(key_list[12], (EXPERTS, FF, D), FF ** -0.5, 0.109375, ((0, 4), (1, 4)))
    return {"queries": queries, "keys": keys, "values": values, "head_bias": head_bias, "documents": documents, "w_out": w_out, "resid": resid, "norm_gain": norm_gain, "expert_ids": expert_ids, "expert_gates": expert_gates, "w_gate": w_gate, "w_up": w_up, "w_down": w_down}


def rounded(array):
    return lax.optimization_barrier(array.astype(jnp.bfloat16)).astype(jnp.float32)

def reference(queries, keys, values, head_bias, documents, w_out, resid, norm_gain, expert_ids, expert_gates, w_gate, w_up, w_down):
    highest = lax.Precision.HIGHEST
    group_size = HEADS // KV_HEADS
    scale_factor = DH ** (-0.5)
    query_all = queries.astype(jnp.float32).reshape(SEQ, KV_HEADS, group_size, DH)
    key_all = keys.astype(jnp.float32).reshape(SEQ, KV_HEADS, DH)
    value_all = values.astype(jnp.float32).reshape(SEQ, KV_HEADS, DH)
    bias_grid = head_bias.astype(jnp.float32).reshape(KV_HEADS, group_size)
    positions = jnp.arange(SEQ, dtype=jnp.int32)
    block_rows = math.gcd(SEQ, 256)

    def attend_block(block_index):
        first = block_index * block_rows
        query_block = lax.dynamic_slice_in_dim(query_all, first, block_rows, 0)
        query_pos = first + jnp.arange(block_rows, dtype=jnp.int32)
        query_doc = lax.dynamic_slice_in_dim(documents, first, block_rows, 0)
        live = (positions[None, :] < query_pos[:, None]) & (documents[None, :] == query_doc[:, None])
        logits = jnp.einsum('qgrd,sgd->grqs', query_block, key_all, precision=highest) * scale_factor + bias_grid[:, :, None, None]
        keep = jnp.where(live, jax.nn.log_sigmoid(-logits), 0.0)
        after = lax.cumsum(keep, axis=3, reverse=True) - keep
        weight = rounded(jnp.where(live, jnp.exp(jax.nn.log_sigmoid(logits) + after), 0.0))
        mixed_block = jnp.einsum('grqs,sgd->qgrd', weight, value_all, precision=highest)
        return mixed_block.reshape(block_rows, HEADS * DH).astype(jnp.bfloat16)
    mixed = lax.map(attend_block, jnp.arange(SEQ // block_rows, dtype=jnp.int32)).reshape(SEQ, HEADS * DH)
    share = HEADS * DH // N_TP
    partials = jnp.einsum('sjc,jcd->sjd', mixed.astype(jnp.float32).reshape(SEQ, N_TP, share), w_out.astype(jnp.float32).reshape(N_TP, share, D), precision=highest)
    middle = (resid.astype(jnp.float32) + lax.optimization_barrier(jnp.sum(rounded(partials), axis=1))).astype(jnp.bfloat16)
    middle_value = middle.astype(jnp.float32)
    normed = (middle_value * lax.rsqrt(lax.optimization_barrier(jnp.mean(middle_value * middle_value, axis=1, keepdims=True)) + 1e-06) * norm_gain.astype(jnp.float32)).astype(jnp.bfloat16)
    assignments = SEQ * TOPK
    most_rows = N_SP * N_TP * CAP
    flat_ids = expert_ids.reshape(-1)
    hidden_share = FF // N_TP

    def run_expert(expert):
        picks = jnp.nonzero(flat_ids == expert, size=most_rows, fill_value=assignments)[0].astype(jnp.int32)
        source = normed[jnp.minimum(picks, assignments - 1) // TOPK].astype(jnp.float32)
        gate_value = jnp.dot(source, w_gate[expert].astype(jnp.float32), precision=highest)
        up_value = jnp.dot(source, w_up[expert].astype(jnp.float32), precision=highest)
        hidden = rounded(jax.nn.silu(gate_value) * up_value).reshape(most_rows, N_TP, hidden_share)
        partial_out = jnp.einsum('bjf,jfd->bjd', hidden, w_down[expert].astype(jnp.float32).reshape(N_TP, hidden_share, D), precision=highest)
        return (lax.optimization_barrier(jnp.sum(rounded(partial_out), axis=1)).astype(jnp.bfloat16), picks)
    outputs, picks_all = lax.map(run_expert, jnp.arange(EXPERTS, dtype=jnp.int32))
    routed = jnp.zeros((assignments, D), jnp.bfloat16).at[picks_all.reshape(-1)].set(outputs.reshape(-1, D), mode='drop')
    combined = lax.optimization_barrier(jnp.sum(expert_gates.astype(jnp.float32)[:, :, None] * routed.reshape(SEQ, TOPK, D).astype(jnp.float32), axis=1))
    return (middle_value + combined).astype(jnp.bfloat16)
```

```python
import functools

import jax
import jax.numpy as jnp
from jax import lax
from jax.experimental import pallas as pl
from jax.experimental.pallas import tpu as pltpu
from jax.sharding import PartitionSpec as P

D = 2048
HEADS = 16
KV_HEADS = 8
DH = 128
TOPK = 2


def passed_along(value, axis, steps):
    count = lax.axis_size(axis)
    initial, last = (max(0, -steps), min(count, count - steps))
    return lax.ppermute(value, axis, [(source, source + steps) for source in range(initial, last)])


def attend_terms(query_grid, bias_grid, key_block, value_block, live, carried):
    kv_local = bias_grid.shape[0]
    key_count = key_block.shape[0]
    logits = (
        jnp.einsum(
            "qgrd,sgd->grqs",
            query_grid,
            key_block.reshape(key_count, kv_local, DH),
            preferred_element_type=jnp.float32,
        )
        * DH ** (-0.5)
        + bias_grid[:, :, None, None]
    )
    keep = jnp.where(live, jax.nn.log_sigmoid(-logits), 0.0)
    after = lax.cumsum(keep, axis=3, reverse=True) - keep + carried[:, :, :, None]
    weight = jnp.where(live, jnp.exp(jax.nn.log_sigmoid(logits) + after), 0.0).astype(jnp.bfloat16)
    partial_mix = jnp.einsum(
        "grqs,sgd->qgrd",
        weight,
        value_block.reshape(key_count, kv_local, DH),
        preferred_element_type=jnp.float32,
    )
    return (partial_mix, jnp.sum(keep, axis=3))


def local(
    queries,
    keys,
    values,
    head_bias,
    documents,
    w_out,
    resid,
    norm_gain,
    expert_ids,
    expert_gates,
    w_gate,
    w_up,
    w_down,
):
    tok_count = queries.shape[0]
    kv_local = keys.shape[1] // DH
    group_size = HEADS // KV_HEADS
    sp_count = lax.axis_size("sp")
    tp_count = lax.axis_size("tp")
    sp_index = lax.axis_index("sp")
    query_grid = queries.reshape(tok_count, kv_local, group_size, DH)
    bias_grid = head_bias.reshape(kv_local, group_size)
    doc_here = documents.astype(jnp.bfloat16)
    doc_column = doc_here.reshape(tok_count, 1)
    local_pos = jnp.arange(tok_count, dtype=jnp.int32)
    live_local = (local_pos[None, :] < local_pos[:, None]) & (
        documents[None, :] == documents[:, None]
    )
    zero_carry = jnp.zeros((kv_local, group_size, tok_count), jnp.float32)
    mix_total, carried = attend_terms(query_grid, bias_grid, keys, values, live_local, zero_carry)

    def visit(turn_index, state):
        mix_sum, carry_sum, key_block, value_block, doc_block = state
        key_block, value_block, doc_block = passed_along(
            (key_block, value_block, doc_block), "sp", 1
        )
        live = (doc_block[:, 0][None, :] == doc_here[:, None]) & (sp_index - turn_index >= 0)
        partial_mix, block_keep = attend_terms(
            query_grid, bias_grid, key_block, value_block, live, carry_sum
        )
        return (mix_sum + partial_mix, carry_sum + block_keep, key_block, value_block, doc_block)

    mix_total, carried, key_last, value_last, doc_last = lax.fori_loop(
        1, sp_count, visit, (mix_total, carried, keys, values, doc_column)
    )
    mixed = mix_total.reshape(tok_count, kv_local * group_size * DH).astype(jnp.bfloat16)
    projected = lax.psum_scatter(
        jnp.dot(mixed, w_out, preferred_element_type=jnp.float32).astype(jnp.bfloat16),
        "tp",
        scatter_dimension=0,
        tiled=True,
    ).astype(jnp.float32)
    middle = (resid.astype(jnp.float32) + projected).astype(jnp.bfloat16)
    middle_value = middle.astype(jnp.float32)
    normed = (
        middle_value
        * lax.rsqrt(jnp.mean(middle_value * middle_value, axis=1, keepdims=True) + 1e-06)
        * norm_gain
    ).astype(jnp.bfloat16)
    row_count = normed.shape[0]
    expert_count = w_gate.shape[0] * sp_count
    slot_limit = min(row_count, max(2, 2 * TOPK * row_count // expert_count))
    flat_ids = expert_ids.reshape(-1)
    onehot_ids = (flat_ids[:, None] == jnp.arange(expert_count, dtype=jnp.int32)[None, :]).astype(
        jnp.int32
    )
    earlier = jnp.cumsum(onehot_ids, axis=0) - onehot_ids
    slot_ids = jnp.sum(earlier * onehot_ids, axis=1)
    target = flat_ids * slot_limit + slot_ids
    placing = (
        jnp.arange(expert_count * slot_limit, dtype=jnp.int32)[:, None] == target[None, :]
    ).astype(jnp.bfloat16)
    by_token = jnp.sum(placing.reshape(expert_count * slot_limit, row_count, TOPK), axis=2)
    outgoing = jnp.dot(by_token, normed, preferred_element_type=jnp.float32).astype(jnp.bfloat16)
    outgoing = outgoing.reshape(expert_count, slot_limit, D)
    arrived = lax.all_to_all(outgoing, "sp", split_axis=0, concat_axis=0, tiled=True)
    gathered = lax.all_gather(arrived, "tp", axis=0, tiled=True)
    expert_rows = gathered.reshape(-1, D)
    gate_value = jnp.dot(expert_rows, w_gate[0], preferred_element_type=jnp.float32)
    up_value = jnp.dot(expert_rows, w_up[0], preferred_element_type=jnp.float32)
    hidden = (jax.nn.silu(gate_value) * up_value).astype(jnp.bfloat16)
    partial_out = jnp.dot(hidden, w_down[0], preferred_element_type=jnp.float32)
    summed = lax.psum_scatter(
        partial_out.reshape(tp_count, sp_count * slot_limit, D).astype(jnp.bfloat16),
        "tp",
        scatter_dimension=0,
        tiled=True,
    ).astype(jnp.float32)
    expert_result = summed.reshape(sp_count, slot_limit, D).astype(jnp.bfloat16)
    returned = lax.all_to_all(expert_result, "sp", split_axis=0, concat_axis=0, tiled=True)
    routed = jnp.dot(placing.T, returned.reshape(-1, D), preferred_element_type=jnp.float32)
    combined = jnp.sum(expert_gates[:, :, None] * routed.reshape(row_count, TOPK, D), axis=1)
    return (middle_value + combined).astype(jnp.bfloat16)


MESH = pl.DeviceIdType.MESH


def visiting_orders(count):
    orders = []
    for i in range(count):
        order = [i] + [b for b in range(count) if b != i]
        if i == count - 1:
            order[:2] = order[1::-1]
        if i == 0 and count > 3:
            order[-2:] = order[:-3:-1]
        orders.append(order)
    return orders


def fused_kernel(
    sp_count,
    tp_count,
    q_hbm,
    k_hbm,
    v_hbm,
    bias_hbm,
    doc_hbm,
    resid_hbm,
    gain_hbm,
    ids_hbm,
    gates_hbm,
    w_out_hbm,
    w_gate_hbm,
    w_up_hbm,
    w_down_hbm,
    out_ref,
    q_ref,
    k_ref,
    v_ref,
    bias_ref,
    doc_ref,
    resid_ref,
    gain_ref,
    ids_ref,
    gates_ref,
    w_out,
    w_gate,
    w_up,
    w_down,
    k_all,
    v_all,
    doc_all,
    mix_acc,
    carry,
    mixed,
    middle,
    x_all,
    hidden,
    part,
    sib_in,
    x_out,
    x_in,
    z_out,
    returned,
    w_sem,
    kv_send,
    kv_recv,
    z_send,
    z_recv,
    gx_send,
    gx_recv,
    gs_send,
    gs_recv,
    ps_send,
    ps_recv,
    px_send,
    px_recv,
    rz_send,
    rz_recv,
):
    s = lax.axis_index("sp")
    t = lax.axis_index("tp")
    width = tp_count // 2
    x, c = t // 2, lax.rem(t, 2)
    sibling = 2 * x + 1 - c
    tok = q_ref.shape[0]
    kv_local = k_ref.shape[1] // DH
    rep = q_ref.shape[1] // k_ref.shape[1]
    rows, model = resid_ref.shape
    ff = w_up.shape[1]
    f32, bf16 = jnp.float32, jnp.bfloat16

    barrier = pltpu.get_barrier_semaphore()
    for j in range(1, sp_count):
        pl.semaphore_signal(
            barrier, inc=1, device_id={"sp": lax.rem(s + j, sp_count)}, device_id_type=MESH
        )
    for j in range(1, tp_count):
        pl.semaphore_signal(
            barrier, inc=1, device_id={"tp": lax.rem(t + j, tp_count)}, device_id_type=MESH
        )

    moves = (
        (doc_hbm, doc_ref),
        (k_hbm, k_ref),
        (v_hbm, v_ref),
        (q_hbm, q_ref),
        (bias_hbm, bias_ref),
        (resid_hbm, resid_ref),
        (gain_hbm, gain_ref),
        (ids_hbm, ids_ref),
        (gates_hbm, gates_ref),
        (w_out_hbm, w_out),
        (w_gate_hbm.at[0], w_gate),
        (w_up_hbm.at[0], w_up),
        (w_down_hbm.at[0], w_down),
    )
    loads = [
        pltpu.make_async_copy(src, dst, w_sem.at[j]) for j, (src, dst) in enumerate(moves)
    ]
    for load in loads:
        load.start()
    for load in loads[:3]:
        load.wait()
    pl.semaphore_wait(barrier, sp_count + tp_count - 2)

    def remote(src, dst, send, recv, device):
        return pltpu.make_async_remote_copy(
            src_ref=src,
            dst_ref=dst,
            send_sem=send,
            recv_sem=recv,
            device_id=device,
            device_id_type=MESH,
        )

    lane_pieces = [slice(g * DH, (g + 1) * DH) for g in range(kv_local)]

    def passed(hop):
        right = {"sp": lax.rem(s + 1, sp_count)}
        pairs = [(doc_ref if hop == 0 else doc_all.at[hop - 1], doc_all.at[hop])]
        for lanes in lane_pieces:
            for own, slots in ((k_ref, k_all), (v_ref, v_all)):
                source = own.at[:, lanes] if hop == 0 else slots.at[hop - 1, :, lanes]
                pairs.append((source, slots.at[hop, :, lanes]))
        return [
            remote(src, dst, kv_send.at[hop, j], kv_recv.at[hop, j], right)
            for j, (src, dst) in enumerate(pairs)
        ]

    has_right = s < sp_count - 1

    @pl.when(has_right)
    def _():
        for copy in passed(0):
            copy.start()

    at_row = lax.broadcasted_iota(jnp.int32, (tok, tok), 0)
    at_col = lax.broadcasted_iota(jnp.int32, (tok, tok), 1)
    summing = jnp.concatenate(
        [(at_row > at_col).astype(f32), jnp.ones((tok, tok), f32)], axis=1
    ).astype(bf16)
    doc_query = jnp.broadcast_to(doc_ref[...].astype(f32), (tok, tok)).T

    def live_keys(hop):
        docs = doc_ref[...] if hop == 0 else doc_all[hop - 1]
        live = doc_query == jnp.broadcast_to(docs.astype(f32), (tok, tok))
        if hop == 0:
            live = live & (at_col < at_row)
        live_f = jnp.concatenate([live.astype(f32)] * rep, axis=0)
        return live_f > 0.5

    def attend(hop, live_all, groups):
        for g in groups:
            heads = [g * rep + r for r in range(rep)]
            query = jnp.concatenate([q_ref[:, h * DH : (h + 1) * DH] for h in heads], axis=0)
            bias = jnp.concatenate([jnp.broadcast_to(bias_ref[0:1, h : h + 1], (tok, tok)) for h in heads], axis=0)
            lanes = slice(g * DH, (g + 1) * DH)
            key = k_ref[:, lanes] if hop == 0 else k_all[hop - 1, :, lanes]
            value = v_ref[:, lanes] if hop == 0 else v_all[hop - 1, :, lanes]
            logits = (
                lax.dot_general(
                    query, key, (((1,), (1,)), ((), ())), preferred_element_type=f32
                )
                * DH ** (-0.5)
                + bias
            )
            keep_any = -(jnp.maximum(logits, 0.0) + jnp.log1p(jnp.exp(-jnp.abs(logits))))
            keep = jnp.where(live_all, keep_any, 0.0)
            high = keep.astype(bf16)
            rest = keep - high.astype(f32)
            mid = rest.astype(bf16)
            low = (rest - mid.astype(f32)).astype(bf16)
            sums = (
                jnp.dot(high, summing, preferred_element_type=f32)
                + jnp.dot(mid, summing, preferred_element_type=f32)
                + jnp.dot(low, summing, preferred_element_type=f32)
            )
            after, total = sums[:, :tok], sums[:, tok:]
            if hop > 0:
                after = after + carry[g]
                total = total + carry[g]
            carry[g] = total
            weight = jnp.where(live_all, jnp.exp(logits + keep_any + after), 0.0).astype(bf16)
            mix = jnp.dot(weight, value, preferred_element_type=f32)
            mix_acc[g] = mix if hop == 0 else mix_acc[g] + mix

    for load in loads[3:5]:
        load.wait()
    groups = range(kv_local)
    attend(0, live_keys(0), groups)
    for hop in range(1, sp_count):

        @pl.when(has_right & (s >= hop))
        def _():
            onward = passed(hop) if hop < sp_count - 1 else None
            for j, copy in enumerate(passed(hop - 1)):
                copy.wait_recv()
                if onward is not None:
                    onward[j].start()
            attend(hop, live_keys(hop), groups)

        @pl.when(jnp.logical_not(has_right) & (s >= hop))
        def _():
            copies = passed(hop - 1)
            copies[0].wait_recv()
            live = live_keys(hop)
            for g in groups:
                copies[1 + 2 * g].wait_recv()
                copies[2 + 2 * g].wait_recv()
                attend(hop, live, [g])

    for load in loads[5:10]:
        load.wait()
    for g in range(kv_local):
        for r in range(rep):
            h = g * rep + r
            mixed[:, h * DH : (h + 1) * DH] = mix_acc[g, r * tok : (r + 1) * tok, :].astype(bf16)

    cuts = 2
    span = model // cuts
    cols = [slice(h * span, (h + 1) * span) for h in range(cuts)]

    def pair_copies(i, h):
        return [
            remote(
                part.at[i, 2 * j + 1 - c, :, cols[h]],
                sib_in.at[i, j, :, cols[h]],
                ps_send.at[i, j, h],
                ps_recv.at[i, j, h],
                {"tp": sibling},
            )
            for j in range(width)
        ]

    def across_copies(i, h):
        return [
            remote(
                x_out.at[i, j - 1, :, cols[h]],
                x_in.at[i, j - 1, :, cols[h]],
                px_send.at[i, j - 1, h],
                px_recv.at[i, j - 1, h],
                {"tp": 2 * lax.rem(x + j, width) + c},
            )
            for j in range(1, width)
        ]

    def pair_sum(i, at, h):
        return part[i, 2 * at + c, :, cols[h]].astype(f32) + sib_in[i, at, :, cols[h]].astype(f32)

    def sum_pairs(i):
        for h in range(cuts):
            for copy in pair_copies(i, h):
                copy.wait_recv()
            for j, copy in enumerate(across_copies(i, h)):
                x_out[i, j, :, cols[h]] = pair_sum(i, lax.rem(x + j + 1, width), h).astype(bf16)
                copy.start()

    def sum_across(i, h):
        result = pair_sum(i, x, h)
        for j, copy in enumerate(across_copies(i, h)):
            copy.wait_recv()
            result = result + x_in[i, j, :, cols[h]].astype(f32)
        return result

    step = 512 if span % 512 == 0 else span
    steps = span // step

    def into_part(i, left, right):
        for h in range(cuts):

            def piece(n, _):
                columns = pl.ds(pl.multiple_of(n * step, step), step)
                value = jnp.dot(left[...], right[:, columns], preferred_element_type=f32)
                part[i, :, :, columns] = value.astype(bf16).reshape(tp_count, rows, step)
                return 0

            lax.fori_loop(h * steps, (h + 1) * steps, piece, 0)
            for copy in pair_copies(i, h):
                copy.start()

    def along_copy(b, h):
        block = x_all.at[s, t, :, cols[h]]
        return remote(block, block, z_send.at[b, h], z_recv.at[s, h], {"sp": b})

    def along_arrival(b, h):
        block = x_all.at[b, t, :, cols[h]]
        return remote(block, block, z_send.at[b, h], z_recv.at[b, h], {"sp": b})

    def spread_copies(b, h):
        block = x_all.at[b, t, :, cols[h]]
        return [
            remote(
                block,
                block,
                gx_send.at[b, j - 1, h],
                gx_recv.at[b, j - 1, h],
                {"tp": 2 * lax.rem(x + j, width) + c},
            )
            for j in range(1, width)
        ]

    def twin_copy(b, j, h):
        block = x_all.at[b, 2 * lax.rem(x - j + width, width) + c, :, cols[h]]
        return remote(block, block, gs_send.at[b, j, h], gs_recv.at[b, j, h], {"tp": sibling})

    def spread(b, h):
        for copy in spread_copies(b, h):
            copy.start()
        twin_copy(b, 0, h).start()

    relayed = sp_count - 2 if sp_count > 3 else None

    def relay_copy(b, h):
        block = x_all.at[b, t, :, cols[h]]
        return remote(block, block, z_send.at[s, h], z_recv.at[b, h], {"sp": 0})

    def arrive(b):
        for h in range(cuts):
            along_arrival(b, h).wait_recv()
            if b == relayed:
                pl.when(s == 1)(relay_copy(b, h).start)
            spread(b, h)

    def return_copy(b, h):
        return remote(
            z_out.at[b, :, cols[h]],
            returned.at[s, :, cols[h]],
            rz_send.at[b, h],
            rz_recv.at[s, h],
            {"sp": b},
        )

    def return_arrival(e, h):
        block = returned.at[e, :, cols[h]]
        return remote(block, block, rz_send.at[e, h], rz_recv.at[e, h], {"sp": e})

    into_part(sp_count, mixed, w_out)
    sum_pairs(sp_count)
    pl.when(s == sp_count - 1)(functools.partial(arrive, 0))
    for h in range(cuts):
        middle[:, cols[h]] = (
            (resid_ref[:, cols[h]].astype(f32) + sum_across(sp_count, h)).astype(bf16).astype(f32)
        )
    mid_value = middle[...]
    x_all[s, t] = (
        mid_value
        * lax.rsqrt(jnp.mean(mid_value * mid_value, axis=1, keepdims=True) + 1e-06)
        * gain_ref[...]
    ).astype(bf16)

    def send_along(d):
        for h in range(cuts):
            along_copy(d, h).start()

    for d in range(sp_count):
        direct = (s != relayed) | (d > 0) if relayed else True
        pl.when((d < s) & direct)(functools.partial(send_along, d))
    for d in reversed(range(sp_count)):
        pl.when(d > s)(functools.partial(send_along, d))
    for h in range(cuts):
        spread(s, h)

    for load in loads[10:]:
        load.wait()

    f_step = 256 if ff % 256 == 0 else ff
    orders = visiting_orders(sp_count)

    def visited(u):
        b = 0
        for i in range(sp_count):
            for j in range(sp_count):
                b = jnp.where((s == i) & (u == j), orders[i][j], b)
        return b

    def finish(b):
        for h in range(cuts):
            z_out[b, :, cols[h]] = sum_across(b, h).astype(bf16)
            pl.when(b != s)(return_copy(b, h).start)

    def turn(u, _):
        now, before = visited(u), visited(u - 1)
        for i in range(sp_count):
            ahead = 0 if i == 0 else 2 if i == sp_count - 1 else 1
            for j, b in enumerate(orders[i]):
                if b == i or (i == sp_count - 1 and b == 0):
                    continue
                at = max(0, min(j - ahead, sp_count - 2))
                pl.when((s == i) & (u == at))(functools.partial(arrive, b))
        pl.when((u > 0) & (u < sp_count - 1))(functools.partial(sum_pairs, before))
        pl.when((u > 1) & (u < sp_count - 1))(functools.partial(finish, visited(u - 2)))
        for h in range(cuts):
            for j, copy in enumerate(spread_copies(now, h)):
                copy.wait_recv()
                twin_copy(now, j + 1, h).start()
        pl.when(u == sp_count - 1)(functools.partial(sum_pairs, before))
        for h in range(cuts):
            for j in range(width):
                twin_copy(now, j, h).wait_recv()

        rows_in = x_all[now].reshape(tp_count * rows, model)

        def widen(n, _):
            columns = pl.ds(pl.multiple_of(n * f_step, f_step), f_step)
            gate = jnp.dot(rows_in, w_gate[:, columns], preferred_element_type=f32)
            up = jnp.dot(rows_in, w_up[:, columns], preferred_element_type=f32)
            hidden[:, columns] = (gate / (1.0 + jnp.exp(-gate)) * up).astype(bf16)
            return 0

        lax.fori_loop(0, ff // f_step, widen, 0)
        into_part(now, hidden, w_down)
        return 0

    lax.fori_loop(0, sp_count, turn, 0)
    finish(visited(sp_count - 3))
    sum_pairs(visited(sp_count - 1))
    finish(visited(sp_count - 2))
    finish(visited(sp_count - 1))

    diagonal = lax.broadcasted_iota(jnp.int32, (rows, rows), 0) == lax.broadcasted_iota(
        jnp.int32, (rows, rows), 1
    )
    for e in range(sp_count):
        chosen = ids_ref[...] == e
        gate_row = jnp.sum(jnp.where(chosen, gates_ref[...], 0.0), axis=0, keepdims=True)
        gate = jnp.sum(
            jnp.where(diagonal, jnp.broadcast_to(gate_row, (rows, rows)), 0.0), axis=1, keepdims=True
        )

        @pl.when(e == s)
        def _():
            middle[...] = middle[...] + gate * z_out[s].astype(f32)

        @pl.when(e != s)
        def _():
            for h in range(cuts):
                return_arrival(e, h).wait_recv()
                middle[:, cols[h]] = middle[:, cols[h]] + gate * returned[
                    e, :, cols[h]
                ].astype(f32)

    out_ref[...] = middle[...].astype(bf16)

    for hop in range(sp_count - 1):

        @pl.when(has_right & (s >= hop))
        def _():
            for copy in passed(hop):
                copy.wait_send()

    def drain(i, _):
        for h in range(cuts):
            for copy in pair_copies(i, h) + across_copies(i, h):
                copy.wait_send()

            @pl.when(i < sp_count)
            def _():
                for copy in spread_copies(i, h):
                    copy.wait_send()
                for j in range(width):
                    twin_copy(i, j, h).wait_send()

            @pl.when((i != s) & (i < sp_count))
            def _():
                return_copy(i, h).wait_send()

            direct = (s != relayed) | (i > 0) if relayed else True
            pl.when((i != s) & (i < sp_count) & direct)(along_copy(i, h).wait_send)
            if relayed:
                pl.when((i == s) & (s == 1))(relay_copy(relayed, h).wait_send)

        return 0

    lax.fori_loop(0, sp_count + 1, drain, 0)


def fused(
    queries,
    keys,
    values,
    head_bias,
    documents,
    w_out,
    resid,
    norm_gain,
    expert_ids,
    expert_gates,
    w_gate,
    w_up,
    w_down,
):
    sp_count, tp_count = lax.axis_size("sp"), lax.axis_size("tp")
    width = tp_count // 2
    tok = queries.shape[0]
    kv_local = keys.shape[1] // DH
    rep = queries.shape[1] // keys.shape[1]
    rows, model = resid.shape
    ff = w_up.shape[2]
    bf16, f32 = jnp.bfloat16, jnp.float32
    dma = pltpu.SemaphoreType.DMA
    operands = (
        queries,
        keys,
        values,
        head_bias.reshape(1, -1),
        documents.reshape(1, tok),
        resid,
        norm_gain.reshape(1, model),
        expert_ids.T,
        expert_gates.T,
        w_out,
        w_gate,
        w_up,
        w_down,
    )
    return pl.pallas_call(
        functools.partial(fused_kernel, sp_count, tp_count),
        out_shape=pltpu.VMEM((rows, model), bf16),
        in_specs=[pl.BlockSpec(memory_space=pl.ANY)] * len(operands),
        out_specs=pl.BlockSpec(memory_space=pltpu.VMEM),
        scratch_shapes=[pltpu.VMEM(one.shape, one.dtype) for one in operands[:9]]
        + [
            pltpu.VMEM(w_out.shape, bf16),
            pltpu.VMEM(w_gate.shape[1:], bf16),
            pltpu.VMEM(w_up.shape[1:], bf16),
            pltpu.VMEM(w_down.shape[1:], bf16),
            pltpu.VMEM((sp_count - 1,) + keys.shape, bf16),
            pltpu.VMEM((sp_count - 1,) + values.shape, bf16),
            pltpu.VMEM((sp_count - 1, 1, tok), jnp.int32),
            pltpu.VMEM((kv_local, rep * tok, DH), f32),
            pltpu.VMEM((kv_local, rep * tok, tok), f32),
            pltpu.VMEM(queries.shape, bf16),
            pltpu.VMEM((rows, model), f32),
            pltpu.VMEM((sp_count, tp_count, rows, model), bf16),
            pltpu.VMEM((tp_count * rows, ff), bf16),
            pltpu.VMEM((sp_count + 1, tp_count, rows, model), bf16),
            pltpu.VMEM((sp_count + 1, width, rows, model), bf16),
            pltpu.VMEM((sp_count + 1, width - 1, rows, model), bf16),
            pltpu.VMEM((sp_count + 1, width - 1, rows, model), bf16),
            pltpu.VMEM((sp_count, rows, model), bf16),
            pltpu.VMEM((sp_count, rows, model), bf16),
            dma((13,)),
            dma((sp_count - 1, 2 * kv_local + 1)),
            dma((sp_count - 1, 2 * kv_local + 1)),
            dma((sp_count, 2)),
            dma((sp_count, 2)),
            dma((sp_count, width - 1, 2)),
            dma((sp_count, width - 1, 2)),
            dma((sp_count, width, 2)),
            dma((sp_count, width, 2)),
            dma((sp_count + 1, width, 2)),
            dma((sp_count + 1, width, 2)),
            dma((sp_count + 1, width - 1, 2)),
            dma((sp_count + 1, width - 1, 2)),
            dma((sp_count, 2)),
            dma((sp_count, 2)),
        ],
        compiler_params=pltpu.CompilerParams(
            collective_id=0, has_side_effects=True, vmem_limit_bytes=60 * 2**20
        ),
    )(*operands)


def block(*arrays):
    queries, resid, w_gate = arrays[0], arrays[6], arrays[10]
    sp_count, tp_count = lax.axis_size("sp"), lax.axis_size("tp")
    rows = resid.shape[0]
    slots = min(rows, max(2, 2 * TOPK * rows // (w_gate.shape[0] * sp_count)))
    even = tp_count % 2 == 0 and sp_count > 2 and tp_count > 2
    if slots == rows and w_gate.shape[0] == 1 and even and queries.shape[0] == DH:
        return fused(*arrays)
    return local(*arrays)


def solution(mesh):
    return jax.shard_map(
        block,
        mesh=mesh,
        in_specs=(
            P(("grp", "sp"), "tp"),
            P(("grp", "sp"), "tp"),
            P(("grp", "sp"), "tp"),
            P("tp"),
            P(("grp", "sp")),
            P("tp", None),
            P(("grp", "sp", "tp"), None),
            P(),
            P(("grp", "sp", "tp"), None),
            P(("grp", "sp", "tp"), None),
            P("sp", None, "tp"),
            P("sp", None, "tp"),
            P("sp", "tp", None),
        ),
        out_specs=P(("grp", "sp", "tp"), None),
        check_vma=False,
    )
```
